32 devices in a mesh: grp: 2 (over y), fs: 4 (over z), tp: 4 (over x, core).
Axes of the slice: x: 2, y: 2, z: 4, core: 2. Of those that a mesh axis runs over, the one named last changes fastest.
Arguments:
- tokens: bfloat16 [4096, 2048], P(('grp', 'fs', 'tp')), parts along dimension 0, may hold values from -6 to 6
- up_master: float32 [2048, 4096], P('fs', 'tp'), may hold values from -0.125 to 0.125
- down_master: float32 [4096, 2048], P('fs', 'tp'), may hold values from -0.09375 to 0.09375
- norm_gain: float32 [2048], P('fs'), may hold values from 0.1 to 1.9
Outputs:
- up_weights: bfloat16 [4096, 4096], P('grp', 'tp'), parts along dimension 0
- down_weights: bfloat16 [8192, 2048], P(('grp', 'tp')), parts along dimension 0
- mlp_output: bfloat16 [4096, 2048], P(('grp', 'fs', 'tp')), parts along dimension 0
The draws below stay inside these ranges and needn't reach their ends.
There are 2 independent parts, one for each index of `grp`. The reference program is written for one: setup_inputs(seed, part) draws one part's arguments, and reference() takes and returns one part's arrays. A program takes and returns all parts, laid end to end along the dimension named above; an argument that names none is the same for every part. Nothing has to cross between parts.
All inputs are finite; a program needn't handle non-finite values.
Results may differ from the reference program's by a relative error of at most 0.014.
Values may be sent and summed in bfloat16 or wider, within the bound.
No kernel may reach another device: no remote copies, remote signals or barrier semaphores. Data moves between devices by JAX's collectives and lax.ppermute only.
A program may use at most 64 MiB of HBM per device.

```python
import jax
import jax.numpy as jnp
from jax import lax

D = 2048
FF = 4096
TOKENS = 2048
N_TP = 4


def steps_of(stream_key, dims, split, smallest, top_value):
    level = 1.0
    for dim, blocks in split:
        steps = jax.random.uniform(jax.random.fold_in(jax.random.fold_in(stream_key, 6), dim), (blocks,), jnp.float32, smallest / len(split), top_value / len(split))
        level = level * jnp.repeat(jnp.exp(steps), dims[dim] // blocks).reshape((-1,) + (1,) * (len(dims) - 1 - dim))
    return level


def centred(stream_key, shape, deviation, bound, cuts=(), dtype=jnp.bfloat16):
    entries = deviation * jax.random.normal(stream_key, shape, jnp.float32)
    if cuts:
        entries = entries * steps_of(stream_key, shape, cuts, -0.22, 0.18)
    return jnp.clip(entries, -bound, bound).astype(dtype)


def setup_inputs(seed: int = 0, part: int = 0) -> dict:
    keys = jax.random.split(jax.random.key(seed), 5)
    part_splits = jax.random.split(jax.random.fold_in(keys[4], part), 5)
    tokens = centred(part_splits[0], (TOKENS, D), 1.0, 6.0, ((0, 16),))
    up_master = centred(keys[1], (D, FF), D ** -0.5, 0.125, ((0, 4), (1, 4)), jnp.float32)
    down_master = centred(keys[2], (FF, D), FF ** -0.5, 0.09375, ((0, 4), (1, 4)), jnp.float32)
    norm_gain = jnp.clip(1.0 + 0.18 * jax.random.normal(keys[3], (D,), jnp.float32), 0.1, 1.9)
    return dict(tokens=tokens, up_master=up_master, down_master=down_master, norm_gain=norm_gain)


def reference(tokens, up_master, down_master, norm_gain):
    up_weights = (norm_gain[:, None] * up_master).astype(jnp.bfloat16)
    down_weights = down_master.astype(jnp.bfloat16)
    float_tokens = tokens.astype(jnp.float32)
    scale = lax.rsqrt(lax.optimization_barrier(jnp.mean(float_tokens * float_tokens, axis=-1, keepdims=True)) + 1e-06)
    normed = (float_tokens * scale).astype(jnp.bfloat16)
    preact = jnp.dot(normed, up_weights, preferred_element_type=jnp.float32)
    rectified = jax.nn.relu(preact)
    hidden = (rectified * rectified).astype(jnp.bfloat16)
    row_total = hidden.shape[0]
    block_width = FF // N_TP
    hidden_blocks = hidden.reshape(row_total, N_TP, block_width).transpose(1, 0, 2)
    down_blocks = down_weights.reshape(N_TP, block_width, D)

    def accumulate(running, operands):
        hidden_block, down_block = operands
        partial_value = jnp.dot(hidden_block, down_block, preferred_element_type=jnp.float32).astype(jnp.bfloat16)
        partial_value = lax.optimization_barrier(partial_value)
        return (running + partial_value.astype(jnp.float32), None)
    start_sum = jnp.zeros((row_total, D), jnp.float32)
    summed, _ = lax.scan(accumulate, start_sum, (hidden_blocks, down_blocks))
    return (up_weights, down_weights, summed.astype(jnp.bfloat16))
```

```python
import functools

import jax
import jax.numpy as jnp
from jax import lax
from jax.experimental import pallas as pl
from jax.experimental.pallas import tpu as pltpu
from jax.sharding import PartitionSpec as P

AXES = ("grp", "fs", "tp")
PIECES = 2


def move(mesh, x, to):
    ng, nf, nt = (mesh.shape[a] for a in AXES)
    pairs = []
    for g in range(ng):
        for f in range(nf):
            for t in range(nt):
                h, e, s = to(g, f, t)
                pairs.append(((g * nf + f) * nt + t, (h * nf + e) * nt + s))
    return lax.ppermute(x, AXES, pairs)


def bits_of(n):
    return [1 << i for i in range(n.bit_length() - 1)]


def row_order(n):
    order = [0]
    for bit in reversed(bits_of(n)):
        order = order + [k | bit for k in order]
    return order


def up_kernel(nf, half, place_ref, normed_ref, own_ref, *refs):
    held, (out_ref, hidden_ref, acc_ref, sems) = refs[: 2 * (nf - 1)], refs[2 * (nf - 1) :]
    g, f = place_ref[0], place_ref[1]
    block = 2 * half
    copies = [pltpu.make_async_copy(own_ref, out_ref.at[pl.ds(pl.multiple_of(f * block, block), block)], sems.at[0])]
    starts = []
    for s in range(1, nf):
        k = lax.rem(f - s + nf, nf)
        for side in range(2):
            h = g if side == 0 else 1 - g
            i = 2 * (s - 1) + side
            start = pl.multiple_of(k * block + h * half, half)
            starts.append((held[i], start))
            copies.append(pltpu.make_async_copy(held[i], out_ref.at[pl.ds(start, half)], sems.at[i + 1]))
    for c in copies:
        c.start()
    own_cols = normed_ref[:, pl.ds(pl.multiple_of(f * block, block), block)]
    acc_ref[...] = jnp.dot(own_cols, own_ref[...], preferred_element_type=jnp.float32)
    for ref, start in starts:
        cols = normed_ref[:, pl.ds(start, half)]
        acc_ref[...] += jnp.dot(cols, ref[...], preferred_element_type=jnp.float32)
    width = acc_ref.shape[1] // 2
    for side in range(2):
        h = g if side == 0 else 1 - g
        r = jnp.maximum(acc_ref[:, pl.ds(pl.multiple_of(h * width, width), width)], 0.0)
        hidden_ref[:, pl.ds(side * width, width)] = (r * r).astype(hidden_ref.dtype)
    for c in copies:
        c.wait()


def down_kernel(nt, piece, width, place_ref, hidden_ref, *refs):
    here, there, (*_, out_ref, part_ref, sems) = refs[:nt], refs[nt : 2 * nt], refs[2 * nt :]
    g, t = place_ref[0], place_ref[2]
    rows, cols = here[0].shape
    copies = []
    for r in range(nt):
        b = t ^ r
        for side, ref in enumerate((here[r], there[r])):
            h = g if side == 0 else 1 - g
            to = out_ref.at[
                pl.ds(pl.multiple_of(h * rows, rows), rows),
                pl.ds(pl.multiple_of(b * width + piece * cols, cols), cols),
            ]
            copies.append(pltpu.make_async_copy(ref, to, sems.at[2 * r + side]))
    for c in copies:
        c.start()
    for r in range(nt):
        total = jnp.dot(hidden_ref[:, :rows], here[r][...], preferred_element_type=jnp.float32)
        total += jnp.dot(hidden_ref[:, rows:], there[r][...], preferred_element_type=jnp.float32)
        part_ref[:, r * cols : (r + 1) * cols] = total.astype(part_ref.dtype)
    for c in copies:
        c.wait()


def shared_halves(mesh, tokens, up_master, down_master, norm_gain):
    nf, nt = mesh.shape["fs"], mesh.shape["tp"]
    g, f, t = (lax.axis_index(a) for a in AXES)
    place = jnp.stack([g, f, t]).astype(jnp.int32)
    send = functools.partial(move, mesh)
    bits = bits_of(nt)
    bf16 = jnp.bfloat16

    float_tokens = tokens.astype(jnp.float32)
    scale = lax.rsqrt(jnp.mean(float_tokens * float_tokens, axis=-1, keepdims=True) + 1e-06)
    blocks = {0: (float_tokens * scale).astype(bf16)}
    for bit in reversed(bits):
        for r in list(blocks):
            blocks[r | bit] = send(blocks[r], lambda a, b, c, bit=bit: (a, b, c ^ bit))
    normed = jnp.concatenate([blocks[r] for r in row_order(nt)], axis=0)

    up_local = (norm_gain[:, None] * up_master).astype(bf16)
    half = up_local.shape[0] // 2
    ring_right = lambda a, b, c: (a, (b + 1) % nf, c)
    ring_left = lambda a, b, c: (a, (b - 1) % nf, c)
    across = lambda a, b, c: (1 - a, b, c)

    def ring(x):
        slots = [x] + [None] * (nf - 1)
        for s in range(1, nf // 2 + 1):
            slots[s] = send(slots[s - 1], ring_right)
        for s in range(nf - 1, nf // 2, -1):
            slots[s] = send(slots[(s + 1) % nf], ring_left)
        return slots

    slots = ring(lax.dynamic_slice_in_dim(up_local, g * half, half, 0))
    held = []
    for s in range(1, nf):
        held += [slots[s], send(slots[s], across)]

    rows, width = down_master.shape[0] // 2, down_master.shape[1]
    cols = width // PIECES
    mine = lax.dynamic_slice_in_dim(down_master, g * rows, rows, 0)
    pieces = []
    for j in range(PIECES):
        slots = ring(mine[:, j * cols : (j + 1) * cols].astype(bf16))
        stack = jnp.stack(slots)
        pick = lambda a: lax.dynamic_index_in_dim(stack, lax.rem(f - a + nf, nf), 0, keepdims=False)
        here = [pick(t)]
        for r in range(1, nt):
            here.append(send(pick(t ^ r), lambda a, b, c, r=r: (a, b, c ^ r)))
        there = [send(h, across) for h in here]
        pieces.append((here, there))

    smem = pl.BlockSpec(memory_space=pltpu.SMEM)
    vmem = pl.BlockSpec(memory_space=pltpu.VMEM)
    anywhere = pl.BlockSpec(memory_space=pl.ANY)
    n_tok, d = normed.shape
    ff = up_local.shape[1]
    up_weights, hidden = pl.pallas_call(
        functools.partial(up_kernel, nf, half),
        out_shape=(jax.ShapeDtypeStruct((d, ff), bf16), jax.ShapeDtypeStruct((n_tok, ff), bf16)),
        in_specs=[smem] + [vmem] * (2 * nf),
        out_specs=(anywhere, vmem),
        scratch_shapes=[pltpu.VMEM((n_tok, ff), jnp.float32), pltpu.SemaphoreType.DMA((2 * nf - 1,))],
        cost_estimate=pl.CostEstimate(flops=2 * n_tok * d * ff, bytes_accessed=4 * d * ff, transcendentals=0),
        name="up",
    )(place, normed, up_local, *held)

    down_shape = jax.ShapeDtypeStruct((2 * rows, width * nt), bf16)
    down_weights = None
    outs = []
    for j, (here, there) in enumerate(pieces):
        carried = [] if down_weights is None else [down_weights]
        down_weights, part = pl.pallas_call(
            functools.partial(down_kernel, nt, j, width),
            out_shape=(down_shape, jax.ShapeDtypeStruct((n_tok, cols * nt), bf16)),
            in_specs=[smem] + [vmem] * (2 * nt + 1) + [anywhere] * len(carried),
            out_specs=(anywhere, vmem),
            scratch_shapes=[pltpu.SemaphoreType.DMA((2 * nt,))],
            input_output_aliases={2 * nt + 2: 0} if carried else {},
            cost_estimate=pl.CostEstimate(
                flops=4 * n_tok * rows * cols * nt, bytes_accessed=8 * rows * cols * nt, transcendentals=0
            ),
            name=f"down{j}",
        )(place, hidden, *here, *there, *carried)
        total = part.astype(jnp.float32)
        for bit in bits:
            keep = total.shape[0] // 2
            got = send(total[keep:].astype(bf16), lambda a, b, c, bit=bit: (a, b, c ^ bit))
            got = jnp.concatenate([got[:, (r ^ bit) * cols : ((r ^ bit) + 1) * cols] for r in range(nt)], axis=1)
            total = total[:keep] + got.astype(jnp.float32)
        outs.append(total.astype(bf16))

    final = []
    by_block = [[o[:, r * cols : (r + 1) * cols] for o in outs] for r in range(nt)]
    by_block = [jnp.concatenate(o, axis=1) for o in by_block]
    for bit in bits:
        odd = (t & bit) != 0
        by_block = [jnp.where(odd, by_block[r ^ bit], by_block[r]) for r in range(nt)]
    mlp_output = jnp.concatenate(by_block, axis=1)
    return up_weights, down_weights, mlp_output


def plain(mesh, tokens, up_master, down_master, norm_gain):
    up_local = (norm_gain[:, None] * up_master).astype(jnp.bfloat16)
    down_local = down_master.astype(jnp.bfloat16)
    float_tokens = tokens.astype(jnp.float32)
    scale = lax.rsqrt(jnp.mean(float_tokens * float_tokens, axis=-1, keepdims=True) + 1e-06)
    normed_local = (float_tokens * scale).astype(jnp.bfloat16)
    normed = lax.all_gather(normed_local, "tp", axis=0, tiled=True)
    up_weights = lax.all_gather(up_local, "fs", axis=0, tiled=True)
    preact = jnp.dot(normed, up_weights, preferred_element_type=jnp.float32)
    gathered_rows = lax.all_gather(down_local, "fs", axis=0, tiled=True)
    down_weights = lax.all_to_all(gathered_rows, "tp", split_axis=0, concat_axis=1, tiled=True)
    rectified = jax.nn.relu(preact)
    hidden = (rectified * rectified).astype(jnp.bfloat16)
    mlp_output = lax.psum_scatter(
        jnp.dot(hidden, down_weights, preferred_element_type=jnp.float32).astype(jnp.bfloat16),
        "tp",
        scatter_dimension=0,
        tiled=True,
    )
    return (up_weights, down_weights, mlp_output)


def solution(mesh):
    ng, nf, nt = (mesh.shape[a] for a in AXES)
    shares = ng == 2 and nf == nt and nt & (nt - 1) == 0
    in_specs = (P(("grp", "fs", "tp"), None), P("fs", "tp"), P("fs", "tp"), P("fs"))
    out_specs = (P("grp", "tp"), P(("grp", "tp"), None), P(("grp", "fs", "tp"), None))
    return jax.shard_map(
        functools.partial(shared_halves if shares else plain, mesh),
        mesh=mesh,
        in_specs=in_specs,
        out_specs=out_specs,
        check_vma=False,
    )
```
